32 devices in a mesh: ep: 8 (over z, y), tp: 4 (over x, core).
Axes of the slice: x: 2, y: 2, z: 4, core: 2. Of those that a mesh axis runs over, the one named last changes fastest.
Arguments:
- tokens: bfloat16 [192, 2048], P('ep'), may hold values from -6 to 6
- delta_state: float32 [192, 8, 128, 128], P('ep', 'tp'), may hold values from -3 to 3
- first_gain: bfloat16 [2048], replicated, may hold values from 0.099609375 to 1.8984375
- query_weight: bfloat16 [2048, 1024], P(None, 'tp'), may hold values from -0.125 to 0.125
- key_weight: bfloat16 [2048, 1024], P(None, 'tp'), may hold values from -0.125 to 0.125
- value_weight: bfloat16 [2048, 1024], P(None, 'tp'), may hold values from -0.125 to 0.125
- outgate_weight: bfloat16 [2048, 1024], P(None, 'tp'), may hold values from -0.125 to 0.125
- beta_weight: bfloat16 [2048, 8], replicated, may hold values from -0.125 to 0.125
- decay_weight: bfloat16 [2048, 8], replicated, may hold values from -0.125 to 0.125
- decay_rate: float32 [8], replicated, may hold values from 0.05 to 4
- decay_bias: float32 [8], replicated, may hold values from -3 to 3
- head_gain: bfloat16 [128], replicated, may hold values from 0.099609375 to 1.8984375
- out_weight: bfloat16 [1024, 2048], P('tp'), may hold values from -0.1875 to 0.1875
- second_gain: bfloat16 [2048], replicated, may hold values from 0.099609375 to 1.8984375
- blend_weight: bfloat16 [2048], replicated, may hold values from -0.125 to 0.125
- dense_gate_weight: bfloat16 [2048, 2048], P(None, 'tp'), may hold values from -0.125 to 0.125
- dense_up_weight: bfloat16 [2048, 2048], P(None, 'tp'), may hold values from -0.125 to 0.125
- dense_down_weight: bfloat16 [2048, 2048], P('tp'), may hold values from -0.125 to 0.125
- expert_gate: bfloat16 [32, 2048, 512], P(('ep', 'tp')), may hold values from -0.125 to 0.125
- expert_up: bfloat16 [32, 2048, 512], P(('ep', 'tp')), may hold values from -0.125 to 0.125
- expert_down: bfloat16 [32, 512, 2048], P(('ep', 'tp')), may hold values from -0.25 to 0.25
- route_ids: int32 [192, 6], P('ep'), may hold values from 0 to 31, all different within a row; in each aligned block of 24 rows (0 to 23, 24 to 47, ...) at most 7 rows name the same one
- route_weights: float32 [192, 6], P('ep'), may hold values from 0.1 to 1
Outputs:
- new_tokens: bfloat16 [192, 2048], P('ep')
- new_state: float32 [192, 8, 128, 128], P('ep', 'tp')
The draws below stay inside these ranges and needn't reach their ends.
Inputs may be any that keep to these rules, and one draw needn't show every extreme that they name: `route_ids`: each row names 6 different experts. In each aligned block of 24 rows (the sequences of one index of ep) no expert is named by more than 7 rows, and in some block an expert is named by exactly 7 rows.
All inputs are finite; a program needn't handle non-finite values.
Results may differ from the reference program's by a relative error of at most 0.017.
Values may be sent and summed in bfloat16 or wider, within the bound.
No kernel may reach another device: no remote copies, remote signals or barrier semaphores. Data moves between devices by JAX's collectives and lax.ppermute only.
A program may use at most 128 MiB of HBM per device.

```python
import math
import jax
import jax.numpy as jnp
import numpy as np
from jax import lax

D = 2048
HEADS = 8
HD = 128
DFF = 2048
DE = 512
TOP_K = 6
SEQ_DEV = 24
TOKENS = 192
EXPERTS = 32
CAP = 7
N_EP = 8


def block_levels(rng, shape, cuts, low, high):
    def one(position, shards_of):
        draws = jax.random.uniform(jax.random.fold_in(jax.random.fold_in(rng, 6), position), (shards_of,), jnp.float32, low / len(cuts), high / len(cuts))
        return jnp.repeat(jnp.exp(draws), shape[position] // shards_of).reshape((-1,) + (1,) * (len(shape) - position - 1))

    loudness = one(*cuts[0])
    for cut in cuts[1:]:
        loudness = loudness * one(*cut)
    return loudness


def shared_out(rng, own, number, rows, number_of, top, reach, lean):
    ranking = jax.random.permutation(rng, number_of)
    crowded, common = shares(number_of, rows * top, reach, lean, True), shares(number_of, rows * top, reach, lean, False)
    places = jnp.arange(number_of)

    def named(sizes, turn):
        used = int((sizes > 0).sum())
        fixed = max(1, used // 4)
        passed = fixed + (places - fixed + turn * (used - fixed)) % max(1, number_of - fixed)
        return jnp.zeros((number_of,), jnp.int32).at[ranking[jnp.where(places < fixed, places, passed)]].set(jnp.asarray(sizes, jnp.int32))

    sizes = jnp.where(number % 4 == 0, named(crowded, number // 4), named(common, number - number // 4 - 1))
    mixed = jax.random.permutation(jax.random.fold_in(own, 3), number_of)
    donor, taker = mixed[0:number_of // 2 * 2:2], mixed[1:number_of // 2 * 2:2]
    margin = jnp.minimum(sizes[donor] - 1, reach - sizes[taker]) // 2
    margin = jnp.where((donor == ranking[0]) | (taker == ranking[0]) | (sizes[taker] == 0), 0, jnp.maximum(margin, 0))
    passed = jax.random.randint(jax.random.fold_in(own, 4), (number_of // 2,), 0, 1 << 20) % (margin + 1)
    sizes = sizes.at[donor].add(-passed).at[taker].add(passed)
    members = jnp.searchsorted(jnp.cumsum(sizes), jnp.arange(rows * top), side="right").astype(jnp.int32)
    listing = members.reshape(top, rows).T
    listing = listing[jax.random.permutation(jax.random.fold_in(own, 1), rows)]
    turn = jax.random.randint(jax.random.fold_in(own, 2), (rows, 1), 0, top)
    return jnp.take_along_axis(listing, (jnp.arange(top)[None, :] + turn) % top, axis=1)


def shares(amount, total, reach, lean, full):
    loads = [(1 << 20) // math.isqrt(standing ** lean) + 1 for standing in range(1, amount + 1)]
    largest = reach if full else min(reach, max(-(-total // amount), total * loads[0] // sum(loads)))
    least = 1 if total - largest >= amount - 1 else 0
    holding, spare = [largest] + [least] * (amount - 1), total - largest - least * (amount - 1)
    while spare > 0:
        movable = [i for i in range(1, amount) if holding[i] < largest] or [i for i in range(1, amount) if holding[i] < reach]
        mass, left = sum([loads[i] for i in movable]), spare
        for i in movable:
            extra = min(reach - holding[i], max(1, left * loads[i] // mass), spare)
            holding[i] = holding[i] + extra
            spare = spare - extra
    return np.array(holding)


def scatter_about(key, dims, spread, limit, pieces=(), kind=jnp.bfloat16):
    factor_of = block_levels(key, dims, pieces, -0.22, 0.18) if pieces else 1.0
    array = jax.random.normal(key, dims, jnp.float32) * spread * factor_of
    return jnp.minimum(jnp.maximum(array, -limit), limit).astype(kind)


def setup_inputs(seed: int = 0) -> dict:
    key_list = jax.random.split(jax.random.key(seed), 24)
    tokens = scatter_about(key_list[0], (TOKENS, D), 1.0, 6.0, ((0, 8),))
    delta_state = scatter_about(key_list[1], (TOKENS, HEADS, HD, HD), 0.3, 3.0, ((0, 8), (1, 4)), jnp.float32)
    first_gain = jnp.clip(1.0 + 0.18 * jax.random.normal(key_list[2], (D,), jnp.float32), 0.099609375, 1.8984375).astype(jnp.bfloat16)
    query_weight = scatter_about(key_list[3], (D, HEADS * HD), D ** -0.5, 0.125, ((1, 4),))
    key_weight = scatter_about(key_list[4], (D, HEADS * HD), D ** -0.5, 0.125, ((1, 4),))
    value_weight = scatter_about(key_list[5], (D, HEADS * HD), D ** -0.5, 0.125, ((1, 4),))
    outgate_weight = scatter_about(key_list[6], (D, HEADS * HD), D ** -0.5, 0.125, ((1, 4),))
    beta_weight = scatter_about(key_list[7], (D, HEADS), D ** -0.5, 0.125)
    decay_weight = scatter_about(key_list[8], (D, HEADS), D ** -0.5, 0.125)
    decay_rate = jnp.clip(jnp.exp(jax.random.uniform(key_list[9], (HEADS,), jnp.float32, math.log(0.05), math.log(4.0))), 0.05, 4.0)
    decay_bias = scatter_about(key_list[10], (HEADS,), 1.0, 3.0, (), jnp.float32)
    head_gain = jnp.clip(1.0 + 0.18 * jax.random.normal(key_list[11], (HD,), jnp.float32), 0.099609375, 1.8984375).astype(jnp.bfloat16)
    out_weight = scatter_about(key_list[12], (HEADS * HD, D), (HEADS * HD) ** -0.5, 0.1875, ((0, 4),))
    second_gain = jnp.clip(1.0 + 0.18 * jax.random.normal(key_list[13], (D,), jnp.float32), 0.099609375, 1.8984375).astype(jnp.bfloat16)
    blend_weight = scatter_about(key_list[14], (D,), D ** -0.5, 0.125)
    dense_gate_weight = scatter_about(key_list[15], (D, DFF), D ** -0.5, 0.125, ((1, 4),))
    dense_up_weight = scatter_about(key_list[16], (D, DFF), D ** -0.5, 0.125, ((1, 4),))
    dense_down_weight = scatter_about(key_list[17], (DFF, D), DFF ** -0.5, 0.125, ((0, 4),))
    expert_gate = scatter_about(key_list[18], (EXPERTS, D, DE), D ** -0.5, 0.125, ((0, 32),))
    expert_up = scatter_about(key_list[19], (EXPERTS, D, DE), D ** -0.5, 0.125, ((0, 32),))
    expert_down = scatter_about(key_list[20], (EXPERTS, DE, D), DE ** -0.5, 0.25, ((0, 32),))
    route_ids_keys = jax.random.split(jax.random.fold_in(key_list[21], 1), TOKENS // SEQ_DEV)
    route_ids_turns = jax.random.permutation(jax.random.fold_in(key_list[21], 3), TOKENS // SEQ_DEV)
    route_ids = jax.vmap(lambda own, number: shared_out(jax.random.fold_in(key_list[21], 2), own, number, SEQ_DEV, EXPERTS, TOP_K, CAP, 2))(route_ids_keys, route_ids_turns).reshape((TOKENS, TOP_K))
    route_weights = jnp.clip(jnp.exp(math.log(1.0) - 2.3025851 * jax.random.uniform(key_list[22], (TOKENS, TOP_K), jnp.float32) ** block_levels(key_list[22], (TOKENS, TOP_K), ((0, 8),), -0.2, 0.2)), 0.1, 1.0)
    return {"tokens": tokens, "delta_state": delta_state, "first_gain": first_gain, "query_weight": query_weight, "key_weight": key_weight, "value_weight": value_weight, "outgate_weight": outgate_weight, "beta_weight": beta_weight, "decay_weight": decay_weight, "decay_rate": decay_rate, "decay_bias": decay_bias, "head_gain": head_gain, "out_weight": out_weight, "second_gain": second_gain, "blend_weight": blend_weight, "dense_gate_weight": dense_gate_weight, "dense_up_weight": dense_up_weight, "dense_down_weight": dense_down_weight, "expert_gate": expert_gate, "expert_up": expert_up, "expert_down": expert_down, "route_ids": route_ids, "route_weights": route_weights}


norm_eps = 1e-06
unit_eps = 1e-06
routed_scale = 2.5

def rms_scale(values, gain):
    values = values.astype(jnp.float32)
    inverse = lax.rsqrt(lax.optimization_barrier(jnp.mean(values * values, axis=-1, keepdims=True)) + norm_eps)
    return values * inverse * gain.astype(jnp.float32)

def unit_rows(values):
    return values * lax.rsqrt(lax.optimization_barrier(jnp.sum(values * values, axis=-1, keepdims=True)) + unit_eps)

def rounded(values):
    return lax.optimization_barrier(values.astype(jnp.bfloat16)).astype(jnp.float32)

def delta_update(delta_state, query_raw, key_raw, value_raw, beta_gate, log_decay):
    head_size = delta_state.shape[-1]
    query_unit = unit_rows(jax.nn.silu(query_raw)) * head_size ** (-0.5)
    key_unit = unit_rows(jax.nn.silu(key_raw))
    value_act = jax.nn.silu(value_raw)
    decayed = jnp.exp(log_decay)[:, :, None, None] * delta_state
    predicted = jnp.einsum('shkv,shk->shv', decayed, key_unit, precision=lax.Precision.HIGHEST)
    update = (beta_gate[:, :, None] * key_unit)[:, :, :, None] * (value_act - predicted)[:, :, None, :]
    new_state = decayed + update
    readout = jnp.einsum('shkv,shk->shv', new_state, query_unit, precision=lax.Precision.HIGHEST)
    return (new_state, readout)

def gated_heads(readout, outgate_raw, head_gain):
    scaled = rms_scale(readout, head_gain) * jax.nn.silu(outgate_raw)
    return scaled.reshape(scaled.shape[0], -1).astype(jnp.bfloat16)

def expert_rows(row_block, gate_mat, up_mat, down_mat):
    gate_part = jnp.dot(row_block, gate_mat, preferred_element_type=jnp.float32)
    up_part = jnp.dot(row_block, up_mat, preferred_element_type=jnp.float32)
    hidden = (jax.nn.silu(gate_part) * up_part).astype(jnp.bfloat16)
    return jnp.dot(hidden, down_mat, preferred_element_type=jnp.float32).astype(jnp.bfloat16)

def routed_sum(normed_mid, expert_gate, expert_up, expert_down, route_ids, route_scale):
    seq_count, model_width = normed_mid.shape
    top_count = route_ids.shape[1]
    per_group = SEQ_DEV * top_count
    grouped = route_ids.reshape(N_EP, per_group).astype(jnp.int32)
    earlier = jnp.arange(per_group)[:, None] > jnp.arange(per_group)[None, :]
    matches = (grouped[:, :, None] == grouped[:, None, :]) & earlier[None]
    rank_of = lax.optimization_barrier(jnp.sum(matches.astype(jnp.int32), axis=2))
    group_ids = jnp.arange(N_EP, dtype=jnp.int32)[:, None]
    expert_slots = N_EP * CAP
    slot_ids = (grouped * expert_slots + group_ids * CAP + rank_of).reshape(-1).astype(jnp.int32)
    token_ids = jnp.arange(seq_count * top_count, dtype=jnp.int32) // top_count
    slot_table = jnp.zeros((EXPERTS * expert_slots,), jnp.int32).at[slot_ids].set(token_ids + 1)
    padded = jnp.concatenate([jnp.zeros((1, model_width), normed_mid.dtype), normed_mid], axis=0)

    def one_expert(inputs):
        index_row, gate_mat, up_mat, down_mat = inputs
        return expert_rows(padded[index_row], gate_mat, up_mat, down_mat)
    outputs = lax.map(one_expert, (slot_table.reshape(EXPERTS, expert_slots), expert_gate, expert_up, expert_down))
    picked = outputs.reshape(-1, model_width)[slot_ids].astype(jnp.float32)
    picked = picked.reshape(seq_count, top_count, model_width)
    return lax.optimization_barrier(jnp.sum(route_scale[:, :, None] * picked, axis=1))

def reference(tokens, delta_state, first_gain, query_weight, key_weight, value_weight, outgate_weight, beta_weight, decay_weight, decay_rate, decay_bias, head_gain, out_weight, second_gain, blend_weight, dense_gate_weight, dense_up_weight, dense_down_weight, expert_gate, expert_up, expert_down, route_ids, route_weights):
    seq_count = tokens.shape[0]
    normed = rms_scale(tokens, first_gain).astype(jnp.bfloat16)

    def project(weight):
        product = jnp.dot(normed, weight, preferred_element_type=jnp.float32)
        return rounded(product).reshape(seq_count, HEADS, HD)
    query_raw = project(query_weight)
    key_raw = project(key_weight)
    value_raw = project(value_weight)
    outgate_raw = project(outgate_weight)
    beta_gate = jax.nn.sigmoid(jnp.dot(normed, beta_weight, preferred_element_type=jnp.float32))
    decay_input = jnp.dot(normed, decay_weight, preferred_element_type=jnp.float32) + decay_bias
    log_decay = -decay_rate * jax.nn.softplus(decay_input)
    new_state, readout = delta_update(delta_state, query_raw, key_raw, value_raw, beta_gate, log_decay)
    gated = gated_heads(readout, outgate_raw, head_gain)
    mixed = jnp.dot(gated, out_weight, preferred_element_type=jnp.float32)
    residual = (tokens.astype(jnp.float32) + mixed).astype(jnp.bfloat16)
    normed_mid = rms_scale(residual, second_gain).astype(jnp.bfloat16)
    blend_gate = jax.nn.sigmoid(jnp.dot(normed_mid, blend_weight, preferred_element_type=jnp.float32))
    dense_gate_raw = jnp.dot(normed_mid, dense_gate_weight, preferred_element_type=jnp.float32)
    dense_up_raw = jnp.dot(normed_mid, dense_up_weight, preferred_element_type=jnp.float32)
    dense_hidden = (jax.nn.silu(dense_gate_raw) * dense_up_raw).astype(jnp.bfloat16)
    dense_out = jnp.dot(dense_hidden, dense_down_weight, preferred_element_type=jnp.float32)
    route_scale = route_weights / lax.optimization_barrier(jnp.sum(route_weights, axis=1, keepdims=True)) * routed_scale
    routed = routed_sum(normed_mid, expert_gate, expert_up, expert_down, route_ids, route_scale)
    combined = residual.astype(jnp.float32) + routed + blend_gate[:, None] * dense_out
    return (combined.astype(jnp.bfloat16), new_state)
```

```python
import jax
import jax.numpy as jnp
from jax import lax
from jax.sharding import PartitionSpec as P

norm_eps = 1e-06
unit_eps = 1e-06
routed_scale = 2.5


def rms_scale(values, gain):
    values = values.astype(jnp.float32)
    inverse = lax.rsqrt(jnp.mean(values * values, axis=-1, keepdims=True) + norm_eps)
    return values * inverse * gain.astype(jnp.float32)


def unit_rows(values):
    return values * lax.rsqrt(jnp.sum(values * values, axis=-1, keepdims=True) + unit_eps)


def rounded(values):
    return lax.optimization_barrier(values.astype(jnp.bfloat16)).astype(jnp.float32)


def delta_update(delta_state, query_raw, key_raw, value_raw, beta_gate, log_decay):
    head_size = delta_state.shape[-1]
    query_unit = unit_rows(jax.nn.silu(query_raw)) * head_size ** (-0.5)
    key_unit = unit_rows(jax.nn.silu(key_raw))
    value_act = jax.nn.silu(value_raw)
    decayed = jnp.exp(log_decay)[:, :, None, None] * delta_state
    predicted = jnp.einsum("shkv,shk->shv", decayed, key_unit, precision=lax.Precision.HIGHEST)
    update = (beta_gate[:, :, None] * key_unit)[:, :, :, None] * (value_act - predicted)[
        :, :, None, :
    ]
    new_state = decayed + update
    readout = jnp.einsum("shkv,shk->shv", new_state, query_unit, precision=lax.Precision.HIGHEST)
    return (new_state, readout)


def gated_heads(readout, outgate_raw, head_gain):
    scaled = rms_scale(readout, head_gain) * jax.nn.silu(outgate_raw)
    return scaled.reshape(scaled.shape[0], -1).astype(jnp.bfloat16)


def tp_sum(part):
    parts = lax.all_gather(part.astype(jnp.bfloat16), "tp", axis=0, tiled=False)
    return jnp.sum(parts.astype(jnp.float32), axis=0)


def expert_rows(row_block, gate_mat, up_mat, down_mat):
    gate_part = jnp.dot(row_block, gate_mat, preferred_element_type=jnp.float32)
    up_part = jnp.dot(row_block, up_mat, preferred_element_type=jnp.float32)
    hidden = (jax.nn.silu(gate_part) * up_part).astype(jnp.bfloat16)
    return jnp.dot(hidden, down_mat, preferred_element_type=jnp.float32).astype(jnp.bfloat16)


def shards(
    tokens,
    delta_state,
    first_gain,
    query_weight,
    key_weight,
    value_weight,
    outgate_weight,
    beta_weight,
    decay_weight,
    decay_rate,
    decay_bias,
    head_gain,
    out_weight,
    second_gain,
    blend_weight,
    dense_gate_weight,
    dense_up_weight,
    dense_down_weight,
    expert_gate,
    expert_up,
    expert_down,
    route_ids,
    route_weights,
):
    seq_count = tokens.shape[0]
    head_local = delta_state.shape[1]
    head_size = delta_state.shape[2]
    top_count = route_ids.shape[1]
    ep_count = lax.axis_size("ep")
    tp_count = lax.axis_size("tp")
    tp_index = lax.axis_index("tp")
    normed = rms_scale(tokens, first_gain).astype(jnp.bfloat16)

    def project(weight):
        product = jnp.dot(normed, weight, preferred_element_type=jnp.float32)
        return rounded(product).reshape(seq_count, head_local, head_size)

    query_raw = project(query_weight)
    key_raw = project(key_weight)
    value_raw = project(value_weight)
    outgate_raw = project(outgate_weight)
    head_start = tp_index * head_local
    beta_all = jax.nn.sigmoid(jnp.dot(normed, beta_weight, preferred_element_type=jnp.float32))
    beta_gate = lax.dynamic_slice_in_dim(beta_all, head_start, head_local, 1)
    decay_input = jnp.dot(normed, decay_weight, preferred_element_type=jnp.float32) + decay_bias
    decay_all = -decay_rate * jax.nn.softplus(decay_input)
    log_decay = lax.dynamic_slice_in_dim(decay_all, head_start, head_local, 1)
    new_state, readout = delta_update(
        delta_state, query_raw, key_raw, value_raw, beta_gate, log_decay
    )
    gated = gated_heads(readout, outgate_raw, head_gain)
    mix_part = jnp.dot(gated, out_weight, preferred_element_type=jnp.float32)
    residual = (tokens.astype(jnp.float32) + tp_sum(mix_part)).astype(jnp.bfloat16)
    normed_mid = rms_scale(residual, second_gain).astype(jnp.bfloat16)
    blend_gate = jax.nn.sigmoid(
        jnp.dot(normed_mid, blend_weight, preferred_element_type=jnp.float32)
    )
    dense_gate_raw = jnp.dot(normed_mid, dense_gate_weight, preferred_element_type=jnp.float32)
    dense_up_raw = jnp.dot(normed_mid, dense_up_weight, preferred_element_type=jnp.float32)
    dense_hidden = (jax.nn.silu(dense_gate_raw) * dense_up_raw).astype(jnp.bfloat16)
    dense_part = jnp.dot(dense_hidden, dense_down_weight, preferred_element_type=jnp.float32)
    expert_count = ep_count * tp_count
    capacity = max(2, (3 * seq_count * top_count + 2 * expert_count - 1) // (2 * expert_count))
    flat_ids = route_ids.reshape(-1)
    assign_count = flat_ids.shape[0]
    earlier = jnp.arange(assign_count)[:, None] > jnp.arange(assign_count)[None, :]
    matches = (flat_ids[:, None] == flat_ids[None, :]) & earlier
    rank_of = jnp.sum(matches.astype(jnp.int32), axis=1)
    owned = flat_ids % tp_count == tp_index
    slot_of = jnp.where(owned, flat_ids // tp_count * capacity + rank_of, -1)
    slot_total = ep_count * capacity
    slot_grid = slot_of.reshape(seq_count, top_count)
    slot_range = jnp.arange(slot_total, dtype=jnp.int32)
    dispatch = jnp.any(slot_grid[None, :, :] == slot_range[:, None, None], axis=2).astype(
        jnp.bfloat16
    )
    model_width = normed_mid.shape[1]
    outgoing = jnp.dot(dispatch, normed_mid, preferred_element_type=jnp.float32).astype(
        jnp.bfloat16
    )
    outgoing = outgoing.reshape(ep_count, capacity, model_width)
    arrived = lax.all_to_all(outgoing, "ep", split_axis=0, concat_axis=0, tiled=True)
    result = expert_rows(
        arrived.reshape(-1, model_width), expert_gate[0], expert_up[0], expert_down[0]
    )
    returned = lax.all_to_all(
        result.reshape(arrived.shape), "ep", split_axis=0, concat_axis=0, tiled=True
    )
    returned_rows = returned.reshape(slot_total, model_width)
    route_scale = route_weights / jnp.sum(route_weights, axis=1, keepdims=True) * routed_scale
    spread = jnp.sum(
        jnp.where(slot_grid[:, :, None] == slot_range, route_scale[:, :, None], 0.0), axis=1
    )
    spread_high = lax.reduce_precision(spread, 8, 7)
    routed_part = jnp.dot(
        spread_high.astype(jnp.bfloat16), returned_rows, preferred_element_type=jnp.float32
    ) + jnp.dot(
        (spread - spread_high).astype(jnp.bfloat16),
        returned_rows,
        preferred_element_type=jnp.float32,
    )
    combined = tp_sum(routed_part + blend_gate[:, None] * dense_part)
    new_tokens = (residual.astype(jnp.float32) + combined).astype(jnp.bfloat16)
    return (new_tokens, new_state)


def solution(mesh):
    placed = (
        P("ep", None),
        P("ep", "tp", None, None),
        P(),
        P(None, "tp"),
        P(None, "tp"),
        P(None, "tp"),
        P(None, "tp"),
        P(),
        P(),
        P(),
        P(),
        P(),
        P("tp", None),
        P(),
        P(),
        P(None, "tp"),
        P(None, "tp"),
        P("tp", None),
        P(("ep", "tp"), None, None),
        P(("ep", "tp"), None, None),
        P(("ep", "tp"), None, None),
        P("ep", None),
        P("ep", None),
    )
    return jax.shard_map(
        shards,
        mesh=mesh,
        in_specs=placed,
        out_specs=(P("ep", None), P("ep", "tp", None, None)),
        check_vma=False,
    )
```

```python
import jax
import jax.numpy as jnp
from jax import lax
from jax.sharding import PartitionSpec as P

norm_eps = 1e-06
unit_eps = 1e-06
routed_scale = 2.5


def rms_scale(values, gain):
    values = values.astype(jnp.float32)
    inverse = lax.rsqrt(jnp.mean(values * values, axis=-1, keepdims=True) + norm_eps)
    return values * inverse * gain.astype(jnp.float32)


def unit_rows(values):
    return values * lax.rsqrt(jnp.sum(values * values, axis=-1, keepdims=True) + unit_eps)


def rounded(values):
    return lax.optimization_barrier(values.astype(jnp.bfloat16)).astype(jnp.float32)


def delta_update(delta_state, query_raw, key_raw, value_raw, beta_gate, log_decay):
    head_size = delta_state.shape[-1]
    query_unit = unit_rows(jax.nn.silu(query_raw)) * head_size ** (-0.5)
    key_unit = unit_rows(jax.nn.silu(key_raw))
    value_act = jax.nn.silu(value_raw)
    decay = jnp.exp(log_decay)[:, :, None]
    weighted_key = beta_gate[:, :, None] * key_unit
    predicted = decay * jnp.sum(delta_state * key_unit[:, :, :, None], axis=2)
    carried = decay * jnp.sum(delta_state * query_unit[:, :, :, None], axis=2)
    error = value_act - predicted
    overlap = jnp.sum(weighted_key * query_unit, axis=-1, keepdims=True)
    new_state = decay[:, :, :, None] * delta_state + weighted_key[:, :, :, None] * error[:, :, None, :]
    readout = carried + overlap * error
    return (new_state, readout)


def gated_heads(readout, outgate_raw, head_gain):
    scaled = rms_scale(readout, head_gain) * jax.nn.silu(outgate_raw)
    return scaled.reshape(scaled.shape[0], -1).astype(jnp.bfloat16)


def tp_sum(part):
    parts = lax.all_gather(part.astype(jnp.bfloat16), "tp", axis=0, tiled=False)
    return jnp.sum(parts.astype(jnp.float32), axis=0)


def expert_rows(row_block, gate_mat, up_mat, down_mat):
    gate_part = jnp.dot(row_block, gate_mat, preferred_element_type=jnp.float32)
    up_part = jnp.dot(row_block, up_mat, preferred_element_type=jnp.float32)
    hidden = (jax.nn.silu(gate_part) * up_part).astype(jnp.bfloat16)
    return jnp.dot(hidden, down_mat, preferred_element_type=jnp.float32).astype(jnp.bfloat16)


def shards(
    tokens,
    delta_state,
    first_gain,
    query_weight,
    key_weight,
    value_weight,
    outgate_weight,
    beta_weight,
    decay_weight,
    decay_rate,
    decay_bias,
    head_gain,
    out_weight,
    second_gain,
    blend_weight,
    dense_gate_weight,
    dense_up_weight,
    dense_down_weight,
    expert_gate,
    expert_up,
    expert_down,
    route_ids,
    route_weights,
):
    seq_count = tokens.shape[0]
    head_local = delta_state.shape[1]
    head_size = delta_state.shape[2]
    top_count = route_ids.shape[1]
    ep_count = lax.axis_size("ep")
    tp_count = lax.axis_size("tp")
    tp_index = lax.axis_index("tp")
    normed = rms_scale(tokens, first_gain).astype(jnp.bfloat16)

    def project(weight):
        product = jnp.dot(normed, weight, preferred_element_type=jnp.float32)
        return rounded(product).reshape(seq_count, head_local, head_size)

    query_raw = project(query_weight)
    key_raw = project(key_weight)
    value_raw = project(value_weight)
    outgate_raw = project(outgate_weight)
    head_start = tp_index * head_local
    beta_all = jax.nn.sigmoid(jnp.dot(normed, beta_weight, preferred_element_type=jnp.float32))
    beta_gate = lax.dynamic_slice_in_dim(beta_all, head_start, head_local, 1)
    decay_input = jnp.dot(normed, decay_weight, preferred_element_type=jnp.float32) + decay_bias
    decay_all = decay_rate * -jax.nn.softplus(decay_input)
    log_decay = lax.dynamic_slice_in_dim(decay_all, head_start, head_local, 1)
    new_state, readout = delta_update(
        delta_state, query_raw, key_raw, value_raw, beta_gate, log_decay
    )
    gated = gated_heads(readout, outgate_raw, head_gain)
    mix_part = jnp.dot(gated, out_weight, preferred_element_type=jnp.float32)
    residual = (tokens.astype(jnp.float32) + tp_sum(mix_part)).astype(jnp.bfloat16)
    normed_mid = rms_scale(residual, second_gain).astype(jnp.bfloat16)
    blend_gate = jax.nn.sigmoid(
        jnp.dot(normed_mid, blend_weight, preferred_element_type=jnp.float32)
    )
    dense_gate_raw = jnp.dot(normed_mid, dense_gate_weight, preferred_element_type=jnp.float32)
    dense_up_raw = jnp.dot(normed_mid, dense_up_weight, preferred_element_type=jnp.float32)
    dense_hidden = (jax.nn.silu(dense_gate_raw) * dense_up_raw).astype(jnp.bfloat16)
    dense_part = jnp.dot(dense_hidden, dense_down_weight, preferred_element_type=jnp.float32)
    expert_count = ep_count * tp_count
    capacity = max(2, (3 * seq_count * top_count + 2 * expert_count - 1) // (2 * expert_count))
    if capacity > 4:
        capacity = -(-capacity // 8) * 8
    flat_ids = route_ids.reshape(-1)
    assign_count = flat_ids.shape[0]
    earlier = jnp.arange(assign_count)[:, None] > jnp.arange(assign_count)[None, :]
    matches = (flat_ids[:, None] == flat_ids[None, :]) & earlier
    rank_of = jnp.sum(matches.astype(jnp.int32), axis=1)
    owned = flat_ids % tp_count == tp_index
    slot_of = jnp.where(owned, flat_ids // tp_count * capacity + rank_of, -1)
    slot_total = ep_count * capacity
    slot_grid = slot_of.reshape(seq_count, top_count)
    slot_range = jnp.arange(slot_total, dtype=jnp.int32)
    dispatch = jnp.any(slot_grid[None, :, :] == slot_range[:, None, None], axis=2).astype(
        jnp.bfloat16
    )
    model_width = normed_mid.shape[1]
    outgoing = jnp.dot(dispatch, normed_mid, preferred_element_type=jnp.float32).astype(
        jnp.bfloat16
    )
    outgoing = outgoing.reshape(ep_count, capacity, model_width)
    arrived = lax.all_to_all(outgoing, "ep", split_axis=0, concat_axis=0, tiled=True)
    result = expert_rows(
        arrived.reshape(-1, model_width), expert_gate[0], expert_up[0], expert_down[0]
    )
    returned = lax.all_to_all(
        result.reshape(arrived.shape), "ep", split_axis=0, concat_axis=0, tiled=True
    )
    returned_rows = returned.reshape(slot_total, model_width)
    route_scale = route_weights / jnp.sum(route_weights, axis=1, keepdims=True) * routed_scale
    spread = jnp.sum(
        jnp.where(slot_grid[:, :, None] == slot_range, route_scale[:, :, None], 0.0), axis=1
    )
    spread_high = lax.reduce_precision(spread, 8, 7)
    routed_part = jnp.dot(
        spread_high.astype(jnp.bfloat16), returned_rows, preferred_element_type=jnp.float32
    ) + jnp.dot(
        (spread - spread_high).astype(jnp.bfloat16),
        returned_rows,
        preferred_element_type=jnp.float32,
    )
    combined = tp_sum(routed_part + blend_gate[:, None] * dense_part)
    new_tokens = (residual.astype(jnp.float32) + combined).astype(jnp.bfloat16)
    return (new_tokens, new_state)


def solution(mesh):
    placed = (
        P("ep", None),
        P("ep", "tp", None, None),
        P(),
        P(None, "tp"),
        P(None, "tp"),
        P(None, "tp"),
        P(None, "tp"),
        P(),
        P(),
        P(),
        P(),
        P(),
        P("tp", None),
        P(),
        P(),
        P(None, "tp"),
        P(None, "tp"),
        P("tp", None),
        P(("ep", "tp"), None, None),
        P(("ep", "tp"), None, None),
        P(("ep", "tp"), None, None),
        P("ep", None),
        P("ep", None),
    )
    return jax.shard_map(
        shards,
        mesh=mesh,
        in_specs=placed,
        out_specs=(P("ep", None), P("ep", "tp", None, None)),
        check_vma=False,
    )
```

```python
import jax
import jax.numpy as jnp
from jax import lax
from jax.sharding import PartitionSpec as P

norm_eps = 1e-06
unit_eps = 1e-06
routed_scale = 2.5


def rms_scale(values, gain):
    values = values.astype(jnp.float32)
    inverse = lax.rsqrt(jnp.mean(values * values, axis=-1, keepdims=True) + norm_eps)
    return values * inverse * gain.astype(jnp.float32)


def unit_rows(values):
    return values * lax.rsqrt(jnp.sum(values * values, axis=-1, keepdims=True) + unit_eps)


def rounded(values):
    return lax.optimization_barrier(values.astype(jnp.bfloat16)).astype(jnp.float32)


def delta_update(delta_state, query_raw, key_raw, value_raw, beta_gate, log_decay):
    head_size = delta_state.shape[-1]
    query_unit = unit_rows(jax.nn.silu(query_raw)) * head_size ** (-0.5)
    key_unit = unit_rows(jax.nn.silu(key_raw))
    value_act = jax.nn.silu(value_raw)
    decay = jnp.exp(log_decay)[:, :, None]
    weighted_key = beta_gate[:, :, None] * key_unit
    predicted = decay * jnp.sum(delta_state * key_unit[:, :, :, None], axis=2)
    carried = decay * jnp.sum(delta_state * query_unit[:, :, :, None], axis=2)
    error = value_act - predicted
    overlap = jnp.sum(weighted_key * query_unit, axis=-1, keepdims=True)
    new_state = decay[:, :, :, None] * delta_state + weighted_key[:, :, :, None] * error[:, :, None, :]
    readout = carried + overlap * error
    return (new_state, readout)


def gated_heads(readout, outgate_raw, head_gain):
    scaled = rms_scale(readout, head_gain) * jax.nn.silu(outgate_raw)
    return scaled.reshape(scaled.shape[0], -1).astype(jnp.bfloat16)


def tp_sum(part):
    parts = lax.all_gather(part.astype(jnp.bfloat16), "tp", axis=0, tiled=False)
    return jnp.sum(parts.astype(jnp.float32), axis=0)


def expert_rows(row_block, gate_mat, up_mat, down_mat):
    gate_part = jnp.dot(row_block, gate_mat, preferred_element_type=jnp.float32)
    up_part = jnp.dot(row_block, up_mat, preferred_element_type=jnp.float32)
    hidden = (jax.nn.silu(gate_part) * up_part).astype(jnp.bfloat16)
    return jnp.dot(hidden, down_mat, preferred_element_type=jnp.float32).astype(jnp.bfloat16)


def shards(
    tokens,
    delta_state,
    first_gain,
    query_weight,
    key_weight,
    value_weight,
    outgate_weight,
    beta_weight,
    decay_weight,
    decay_rate,
    decay_bias,
    head_gain,
    out_weight,
    second_gain,
    blend_weight,
    dense_gate_weight,
    dense_up_weight,
    dense_down_weight,
    expert_gate,
    expert_up,
    expert_down,
    route_ids,
    route_weights,
):
    seq_count = tokens.shape[0]
    head_local = delta_state.shape[1]
    head_size = delta_state.shape[2]
    top_count = route_ids.shape[1]
    ep_count = lax.axis_size("ep")
    tp_count = lax.axis_size("tp")
    tp_index = lax.axis_index("tp")
    normed = lax.optimization_barrier(rms_scale(tokens, first_gain).astype(jnp.bfloat16))

    def project(weight):
        product = jnp.dot(normed, weight, preferred_element_type=jnp.float32)
        return rounded(product).reshape(seq_count, head_local, head_size)

    query_raw = project(query_weight)
    key_raw = project(key_weight)
    value_raw = project(value_weight)
    outgate_raw = project(outgate_weight)
    head_start = tp_index * head_local
    beta_all = jax.nn.sigmoid(jnp.dot(normed, beta_weight, preferred_element_type=jnp.float32))
    beta_gate = lax.dynamic_slice_in_dim(beta_all, head_start, head_local, 1)
    decay_input = jnp.dot(normed, decay_weight, preferred_element_type=jnp.float32) + decay_bias
    decay_all = decay_rate * -jax.nn.softplus(decay_input)
    log_decay = lax.dynamic_slice_in_dim(decay_all, head_start, head_local, 1)
    new_state, readout = delta_update(
        delta_state, query_raw, key_raw, value_raw, beta_gate, log_decay
    )
    gated = gated_heads(readout, outgate_raw, head_gain)
    mix_part = jnp.dot(gated, out_weight, preferred_element_type=jnp.float32)
    residual = (tokens.astype(jnp.float32) + tp_sum(mix_part)).astype(jnp.bfloat16)
    normed_mid = lax.optimization_barrier(rms_scale(residual, second_gain).astype(jnp.bfloat16))
    blend_gate = jax.nn.sigmoid(
        jnp.dot(normed_mid, blend_weight, preferred_element_type=jnp.float32)
    )
    dense_gate_raw = jnp.dot(normed_mid, dense_gate_weight, preferred_element_type=jnp.float32)
    dense_up_raw = jnp.dot(normed_mid, dense_up_weight, preferred_element_type=jnp.float32)
    dense_hidden = (jax.nn.silu(dense_gate_raw) * dense_up_raw).astype(jnp.bfloat16)
    dense_part = jnp.dot(dense_hidden, dense_down_weight, preferred_element_type=jnp.float32)
    expert_count = ep_count * tp_count
    capacity = max(2, (3 * seq_count * top_count + 2 * expert_count - 1) // (2 * expert_count))
    if capacity > 4:
        capacity = -(-capacity // 8) * 8
    flat_ids = route_ids.reshape(-1)
    assign_count = flat_ids.shape[0]
    earlier = jnp.arange(assign_count)[:, None] > jnp.arange(assign_count)[None, :]
    matches = (flat_ids[:, None] == flat_ids[None, :]) & earlier
    rank_of = jnp.sum(matches.astype(jnp.int32), axis=1)
    owned = flat_ids % tp_count == tp_index
    slot_of = jnp.where(owned, flat_ids // tp_count * capacity + rank_of, -1)
    slot_total = ep_count * capacity
    slot_grid = slot_of.reshape(seq_count, top_count)
    slot_range = jnp.arange(slot_total, dtype=jnp.int32)
    dispatch = jnp.any(slot_grid[None, :, :] == slot_range[:, None, None], axis=2).astype(
        jnp.bfloat16
    )
    model_width = normed_mid.shape[1]
    outgoing = jnp.dot(dispatch, normed_mid, preferred_element_type=jnp.float32).astype(
        jnp.bfloat16
    )
    outgoing = outgoing.reshape(ep_count, capacity, model_width)
    arrived = lax.all_to_all(outgoing, "ep", split_axis=0, concat_axis=0, tiled=True)
    result = expert_rows(
        arrived.reshape(-1, model_width), expert_gate[0], expert_up[0], expert_down[0]
    )
    returned = lax.all_to_all(
        result.reshape(arrived.shape), "ep", split_axis=0, concat_axis=0, tiled=True
    )
    returned_rows = returned.reshape(slot_total, model_width)
    route_scale = route_weights / jnp.sum(route_weights, axis=1, keepdims=True) * routed_scale
    spread = jnp.sum(
        jnp.where(slot_grid[:, :, None] == slot_range, route_scale[:, :, None], 0.0), axis=1
    )
    spread_high = lax.reduce_precision(spread, 8, 7)
    routed_part = jnp.dot(
        spread_high.astype(jnp.bfloat16), returned_rows, preferred_element_type=jnp.float32
    ) + jnp.dot(
        (spread - spread_high).astype(jnp.bfloat16),
        returned_rows,
        preferred_element_type=jnp.float32,
    )
    combined = tp_sum(routed_part + blend_gate[:, None] * dense_part)
    new_tokens = (residual.astype(jnp.float32) + combined).astype(jnp.bfloat16)
    return (new_tokens, new_state)


def solution(mesh):
    placed = (
        P("ep", None),
        P("ep", "tp", None, None),
        P(),
        P(None, "tp"),
        P(None, "tp"),
        P(None, "tp"),
        P(None, "tp"),
        P(),
        P(),
        P(),
        P(),
        P(),
        P("tp", None),
        P(),
        P(),
        P(None, "tp"),
        P(None, "tp"),
        P("tp", None),
        P(("ep", "tp"), None, None),
        P(("ep", "tp"), None, None),
        P(("ep", "tp"), None, None),
        P("ep", None),
        P("ep", None),
    )
    return jax.shard_map(
        shards,
        mesh=mesh,
        in_specs=placed,
        out_specs=(P("ep", None), P("ep", "tp", None, None)),
        check_vma=False,
    )
```
